32 devices in a mesh: sp: 8 (over z, y), tp: 4 (over x, core).
Axes of the slice: x: 2, y: 2, z: 4, core: 2. Of those that a mesh axis runs over, the one named last changes fastest.
Arguments:
- residual: bfloat16 [8192, 2048], P(('sp', 'tp')), may hold values from -6 to 6
- first_group_queries: bfloat16 [8192, 1024], P('sp', 'tp'), may hold values from -6 to 6
- first_group_keys: bfloat16 [8192, 1024], P('sp', 'tp'), may hold values from -6 to 6
- second_group_queries: bfloat16 [8192, 512], P('sp', 'tp'), may hold values from -6 to 6
- second_group_keys: bfloat16 [8192, 512], P('sp', 'tp'), may hold values from -6 to 6
- primary_retain_switch_inputs: bfloat16 [8192, 1024], P('sp', 'tp'), may hold values from -12 to 16
- secondary_retain_switch_inputs: bfloat16 [8192, 512], P('sp', 'tp'), may hold values from -12 to 16
- timestep_fading_exponent: float32 [8192], P('sp'), may hold values from -2.1 to 0
- values: bfloat16 [2, 8192, 1024], P(None, 'sp', 'tp'), may hold values from -6 to 6
- output_gate_logits: bfloat16 [2, 8192, 1024], P(None, 'sp', 'tp'), may hold values from -6 to 6
- head_norm_gains: float32 [2, 1024], P(None, 'tp'), may hold values from 0.1 to 1.9
- output_projection: bfloat16 [2, 1024, 2048], P(None, 'tp'), may hold values from -0.125 to 0.125
- feedforward_norm_gain: float32 [2048], replicated, may hold values from 0.1 to 1.9
- gate_projection: bfloat16 [2048, 6144], P('sp', 'tp'), may hold values from -0.125 to 0.125
- up_projection: bfloat16 [2048, 6144], P('sp', 'tp'), may hold values from -0.125 to 0.125
- down_projection: bfloat16 [6144, 2048], P('tp', 'sp'), may hold values from -0.078125 to 0.078125
Outputs:
- layer_out: bfloat16 [8192, 2048], P(('sp', 'tp'))
The draws below stay inside these ranges and needn't reach their ends.
All inputs are finite; a program needn't handle non-finite values.
Results may differ from the reference program's by a relative error of at most 0.018.
Values may be sent and summed in bfloat16 or wider, within the bound.
A program may use at most 128 MiB of HBM per device.

```python
import jax
import jax.numpy as jnp
from jax import lax

D = 2048
HEADS = 8
FIRST_KEY_SIZE = 128
SECOND_KEY_SIZE = 64
DV = 128
FF = 6144
BLOCK = 64
SEQ = 8192
N_TP = 4


def forget_draw(base_key, key_width):
    key_rank, key_factor, key_channel, key_jitter, key_long, key_level = jax.random.split(base_key, 6)
    ranking = jax.random.permutation(key_rank, HEADS)
    fast_count = HEADS // 2
    long_share = 0.5
    fast_mask = jnp.repeat((ranking < fast_count).astype(jnp.float32), key_width)
    slow_level = jnp.log(SEQ / 3.2)
    fast_level = -jnp.log(jnp.exp(16.0 / (0.6 * BLOCK)) - 1.0)
    long_mask = (jax.random.uniform(key_long, (HEADS * key_width,), jnp.float32) < long_share).astype(jnp.float32)
    spread_level = jax.random.uniform(key_level, (HEADS * key_width,), jnp.float32, jnp.log(4.0), slow_level)
    slow_channel = long_mask * slow_level + (1.0 - long_mask) * spread_level
    base_level = fast_mask * fast_level + (1.0 - fast_mask) * slow_channel
    factor = jax.random.uniform(key_factor, (SEQ // BLOCK, 1), jnp.float32, 0.0, jnp.log(4.0))
    factor = jnp.repeat(factor, BLOCK, axis=0)
    channel = jnp.clip(0.5 * jax.random.normal(key_channel, (1, HEADS * key_width), jnp.float32), -1.5, 1.5)
    jitter = jnp.clip(0.8 * jax.random.normal(key_jitter, (SEQ, HEADS * key_width), jnp.float32), -3.2, 3.2)
    result = base_level[None, :] - factor + channel + jitter
    return result.astype(jnp.bfloat16)


def draw_primary_retain_switch_inputs(key, part):
    return forget_draw(jax.random.fold_in(key, 11), FIRST_KEY_SIZE)


def draw_secondary_retain_switch_inputs(key, part):
    return forget_draw(jax.random.fold_in(key, 23), SECOND_KEY_SIZE)


def draw_timestep_fading_exponent(key, part):
    key_spot, key_loss = jax.random.split(jax.random.fold_in(key, 37))
    positions = jax.random.randint(key_spot, (3,), 0, SEQ)
    losses = jax.random.uniform(key_loss, (3,), jnp.float32, jnp.log(0.5), jnp.log(0.8))
    hits = jnp.arange(SEQ)[:, None] == positions[None, :]
    return jnp.sum(jnp.where(hits, losses[None, :], 0.0), axis=1).astype(jnp.float32)


def block_scale(stream_key, dims, shards, smallest, top_value):
    factor_of = 1.0
    for dim, shards_of in shards:
        draws = jax.random.uniform(jax.random.fold_in(jax.random.fold_in(stream_key, 6), dim), (shards_of,), jnp.float32, smallest / len(shards), top_value / len(shards))
        factor_of = factor_of * jnp.repeat(jnp.exp(draws), dims[dim] // shards_of).reshape((-1,) + (1,) * (len(dims) - 1 - dim))
    return factor_of


def scatter_about(key, shape, scale, limit, pieces=(), kind=jnp.bfloat16):
    entries = scale * jax.random.normal(key, shape, jnp.float32)
    if pieces:
        entries = entries * block_scale(key, shape, pieces, -0.22, 0.18)
    return jnp.clip(entries, -limit, limit).astype(kind)


def setup_inputs(seed: int = 0) -> dict:
    streams_of = jax.random.split(jax.random.key(seed), 17)
    return {
        "residual": scatter_about(streams_of[0], (SEQ, D), 1.0, 6.0, ((0, 32),)),
        "first_group_queries": scatter_about(streams_of[1], (SEQ, HEADS * FIRST_KEY_SIZE), 1.0, 6.0, ((0, 8), (1, 4))),
        "first_group_keys": scatter_about(streams_of[2], (SEQ, HEADS * FIRST_KEY_SIZE), 1.0, 6.0, ((0, 8), (1, 4))),
        "second_group_queries": scatter_about(streams_of[3], (SEQ, HEADS * SECOND_KEY_SIZE), 1.0, 6.0, ((0, 8), (1, 4))),
        "second_group_keys": scatter_about(streams_of[4], (SEQ, HEADS * SECOND_KEY_SIZE), 1.0, 6.0, ((0, 8), (1, 4))),
        "primary_retain_switch_inputs": draw_primary_retain_switch_inputs(jax.random.fold_in(streams_of[16], 71), 0),
        "secondary_retain_switch_inputs": draw_secondary_retain_switch_inputs(jax.random.fold_in(streams_of[16], 71), 0),
        "timestep_fading_exponent": draw_timestep_fading_exponent(jax.random.fold_in(streams_of[16], 71), 0),
        "values": scatter_about(streams_of[8], (2, SEQ, HEADS * DV), 1.0, 6.0, ((1, 8), (2, 4))),
        "output_gate_logits": scatter_about(streams_of[9], (2, SEQ, HEADS * DV), 1.0, 6.0, ((1, 8), (2, 4))),
        "head_norm_gains": jnp.clip(1.0 + 0.18 * jax.random.normal(streams_of[10], (2, HEADS * DV), jnp.float32), 0.1, 1.9),
        "output_projection": scatter_about(streams_of[11], (2, HEADS * DV, D), (2 * HEADS * DV) ** -0.5, 0.125, ((1, 4),)),
        "feedforward_norm_gain": jnp.clip(1.0 + 0.18 * jax.random.normal(streams_of[12], (D,), jnp.float32), 0.1, 1.9),
        "gate_projection": scatter_about(streams_of[13], (D, FF), D ** -0.5, 0.125, ((0, 8), (1, 4))),
        "up_projection": scatter_about(streams_of[14], (D, FF), D ** -0.5, 0.125, ((0, 8), (1, 4))),
        "down_projection": scatter_about(streams_of[15], (FF, D), FF ** -0.5, 0.078125, ((0, 4), (1, 8))),
    }


EPS = 1e-06
SOFTNESS_SCALE = 16.0
highest_precision = lax.Precision.HIGHEST

def blocks(source, block_count, head_count, key_width):
    return source.astype(jnp.float32).reshape(block_count, BLOCK, head_count, key_width).transpose(0, 2, 1, 3)

def mechanism(query_matrix_rows, key_matrix_rows, value_matrix_rows, decay_logarithm, key_width):
    block_count = query_matrix_rows.shape[0] // BLOCK
    query_blocks = blocks(query_matrix_rows, block_count, HEADS, key_width) * key_width ** (-0.5)
    key_blocks = blocks(key_matrix_rows, block_count, HEADS, key_width)
    value_blocks = blocks(value_matrix_rows, block_count, HEADS, DV)
    decay_blocks = jnp.cumsum(blocks(decay_logarithm, block_count, HEADS, key_width), axis=2)
    causal = jnp.tril(jnp.ones((BLOCK, BLOCK), dtype=bool))

    def advance(running_state, inputs):
        query_piece, key_piece, value_piece, decay_piece = inputs
        spread_log = decay_piece[:, :, None, :] - decay_piece[:, None, :, :]
        decay_grid = jnp.exp(jnp.where(causal[None, :, :, None], spread_log, -jnp.inf))
        scores = lax.optimization_barrier(jnp.sum(query_piece[:, :, None, :] * key_piece[:, None, :, :] * decay_grid, axis=-1))
        block_result = jnp.einsum('hij,hjv->hiv', scores, value_piece, precision=highest_precision)
        block_result = block_result + jnp.einsum('rus,rsp->rup', query_piece * jnp.exp(decay_piece), running_state, precision=highest_precision)
        final_log_decay = decay_piece[:, -1:, :]
        running_state = jnp.exp(final_log_decay[:, 0, :])[:, :, None] * running_state + jnp.einsum('qxe,qxt->qet', key_piece * jnp.exp(final_log_decay - decay_piece), value_piece, precision=highest_precision)
        return (running_state, block_result)
    zero_state = jnp.zeros((HEADS, key_width, DV), jnp.float32)
    _, outputs = lax.scan(advance, zero_state, (query_blocks, key_blocks, value_blocks, decay_blocks))
    return outputs.transpose(0, 2, 1, 3).reshape(query_matrix_rows.shape[0], HEADS, DV)

def gate_heads(head_out, gate_rows, gain_row):
    inverse = lax.rsqrt(lax.optimization_barrier(jnp.mean(head_out * head_out, axis=-1, keepdims=True)) + EPS)
    normed = (head_out * inverse).reshape(head_out.shape[0], -1) * gain_row
    return (jax.nn.silu(gate_rows.astype(jnp.float32)) * normed).astype(jnp.bfloat16)

def grouped_product(left_sides, right_sides):
    portion = left_sides[0].shape[1] // N_TP
    row_count = left_sides[0].shape[0]
    col_count = right_sides[0].shape[1]

    def add_group(group_index, summed):
        offset = (group_index * portion).astype(jnp.int32)
        partial_value = jnp.zeros((row_count, col_count), jnp.float32)
        for left_side, right_side in zip(left_sides, right_sides):
            partial_value = partial_value + jnp.dot(lax.dynamic_slice_in_dim(left_side, offset, portion, 1), lax.dynamic_slice_in_dim(right_side, offset, portion, 0), preferred_element_type=jnp.float32)
        rounded = lax.optimization_barrier(partial_value.astype(jnp.bfloat16))
        return summed + rounded.astype(jnp.float32)
    return lax.fori_loop(0, N_TP, add_group, jnp.zeros((row_count, col_count), jnp.float32))

def row_norm(source, gain_row):
    widened = source.astype(jnp.float32)
    inverse = lax.rsqrt(lax.optimization_barrier(jnp.mean(widened * widened, axis=-1, keepdims=True)) + EPS)
    return (widened * inverse * gain_row).astype(jnp.bfloat16)

def reference(residual, first_group_queries, first_group_keys, second_group_queries, second_group_keys, primary_retain_switch_inputs, secondary_retain_switch_inputs, timestep_fading_exponent, values, output_gate_logits, head_norm_gains, output_projection, feedforward_norm_gain, gate_projection, up_projection, down_projection):
    primary_fading_exponent = jax.nn.log_sigmoid(primary_retain_switch_inputs.astype(jnp.float32)) / SOFTNESS_SCALE + timestep_fading_exponent[:, None]
    secondary_fading_exponent = jax.nn.log_sigmoid(secondary_retain_switch_inputs.astype(jnp.float32)) / SOFTNESS_SCALE + timestep_fading_exponent[:, None]
    heads_a = mechanism(first_group_queries, first_group_keys, values[0], primary_fading_exponent, FIRST_KEY_SIZE)
    heads_b = mechanism(second_group_queries, second_group_keys, values[1], secondary_fading_exponent, SECOND_KEY_SIZE)
    gated_a = gate_heads(heads_a, output_gate_logits[0], head_norm_gains[0])
    gated_b = gate_heads(heads_b, output_gate_logits[1], head_norm_gains[1])
    attention = grouped_product((gated_a, gated_b), (output_projection[0], output_projection[1]))
    mid_rows = (residual.astype(jnp.float32) + attention).astype(jnp.bfloat16)
    normed = row_norm(mid_rows, feedforward_norm_gain)
    gate_sum = jnp.dot(normed, gate_projection, preferred_element_type=jnp.float32)
    up_sum = jnp.dot(normed, up_projection, preferred_element_type=jnp.float32)
    hidden = (jax.nn.silu(gate_sum) * up_sum).astype(jnp.bfloat16)
    down_sum = grouped_product((hidden,), (down_projection,))
    return (mid_rows.astype(jnp.float32) + down_sum).astype(jnp.bfloat16)
```

```python
import jax
import jax.numpy as jnp
from jax import lax
from jax.experimental import pallas as pl
from jax.experimental.pallas import tpu as pltpu
from jax.sharding import PartitionSpec as P

FIRST_KEY_SIZE = 128
SECOND_KEY_SIZE = 64
DV = 128
CHUNK = 128
MIDDLE = CHUNK // 2 - 1
PAD = 16

EPS = 1e-06
SOFTNESS_SCALE = 16.0


def dot(a, b, dims):
    return lax.dot_general(a, b, (dims, ((), ())), preferred_element_type=jnp.float32)


def positions():
    row = lax.broadcasted_iota(jnp.int32, (CHUNK, CHUNK), 0)
    column = lax.broadcasted_iota(jnp.int32, (CHUNK, CHUNK), 1)
    return row, column


def fading_sums(fading_row):
    row, column = positions()
    as_column = jnp.sum(jnp.where(row == column, fading_row, 0.0), axis=1, keepdims=True)
    column_sums = jnp.sum(jnp.where(column <= row, fading_row, 0.0), axis=1, keepdims=True)
    row_sums = jnp.sum(jnp.where(row <= column, as_column, 0.0), axis=0, keepdims=True)
    return column_sums, row_sums


def channel_sums(switches):
    row, column = positions()
    x = switches.astype(jnp.float32)
    logs = (jnp.minimum(x, 0.0) - jnp.log1p(jnp.exp(-jnp.abs(x)))) * (1.0 / SOFTNESS_SCALE)
    lower = (column <= row).astype(jnp.bfloat16)
    high = logs.astype(jnp.bfloat16)
    low = (logs - high.astype(jnp.float32)).astype(jnp.bfloat16)
    return dot(lower, high, ((1,), (0,))) + dot(lower, low, ((1,), (0,)))


def lanes_of(head, width, key_width):
    lane = lax.broadcasted_iota(jnp.int32, (1, width), 1)
    return (lane >= head * key_width) & (lane < (head + 1) * key_width)


def advanced(state, inverse_keys, weighted, sums, total_fading, key_width):
    width = state.shape[1]
    end, middle = sums[CHUNK - 1 :, :], sums[MIDDLE : MIDDLE + 1, :]
    head_count = width // key_width
    if key_width % 128 == 0:
        added = jnp.concatenate(
            [
                dot(
                    weighted[:, h * DV : (h + 1) * DV],
                    inverse_keys[:, h * key_width : (h + 1) * key_width],
                    ((0,), (0,)),
                )
                for h in range(head_count)
            ],
            axis=1,
        )
    else:
        added = jnp.zeros((DV, width), jnp.float32)
        for h in range(head_count):
            product = dot(weighted[:, h * DV : (h + 1) * DV], inverse_keys, ((0,), (0,)))
            added = jnp.where(lanes_of(h, width, key_width), product, added)
    return jnp.exp(end + total_fading) * state + jnp.exp(end - middle) * added


def state_kernel(
    keys_a, keys_b, switches_a, switches_b, fading, values, packed, state_a, state_b, decay
):
    step = pl.program_id(0)
    width_a = keys_a.shape[1]

    @pl.when(step == 0)
    def _():
        state_a[...] = jnp.zeros_like(state_a)
        state_b[...] = jnp.zeros_like(state_b)
        decay[...] = jnp.zeros_like(decay)

    column_sums, _ = fading_sums(fading[0])
    total_fading = column_sums[CHUNK - 1 :, :]
    later = jnp.exp(total_fading - column_sums)
    for group, (keys, switches, state, key_width, start) in enumerate(
        (
            (keys_a, switches_a, state_a, FIRST_KEY_SIZE, 0),
            (keys_b, switches_b, state_b, SECOND_KEY_SIZE, width_a),
        )
    ):
        width = keys.shape[1]
        sums = channel_sums(switches[...])
        middle = sums[MIDDLE : MIDDLE + 1, :]
        inverse_keys = (keys[...].astype(jnp.float32) * jnp.exp(middle - sums)).astype(jnp.bfloat16)
        weighted = (values[group].astype(jnp.float32) * later).astype(jnp.bfloat16)
        state[...] = advanced(state[...], inverse_keys, weighted, sums, total_fading, key_width)
        decay[:, start : start + width] += sums[CHUNK - 1 :, :] + total_fading

    @pl.when(step == pl.num_programs(0) - 1)
    def _():
        packed[:DV, :width_a] = state_a[...].astype(jnp.bfloat16)
        packed[:DV, width_a:] = state_b[...].astype(jnp.bfloat16)
        packed[DV:, :] = jnp.broadcast_to(jnp.exp(decay[:1, :]), (PAD, decay.shape[1])).astype(
            jnp.bfloat16
        )


def output_kernel(
    place,
    everything,
    queries_a,
    queries_b,
    keys_a,
    keys_b,
    switches_a,
    switches_b,
    fading,
    values,
    gates,
    gains,
    projection,
    out,
    state_a,
    state_b,
):
    step = pl.program_id(0)
    width_a = keys_a.shape[1]

    @pl.when(step == 0)
    def _():
        state_a[...] = jnp.zeros_like(state_a)
        state_b[...] = jnp.zeros_like(state_b)

        @pl.loop(0, place[0])
        def _(k):
            part = everything[k].astype(jnp.float32)
            factor = part[DV : DV + 1, :]
            state_a[...] = factor[:, :width_a] * state_a[...] + part[:DV, :width_a]
            state_b[...] = factor[:, width_a:] * state_b[...] + part[:DV, width_a:]

    row, column = positions()
    causal = column <= row
    column_sums, row_sums = fading_sums(fading[0])
    total_fading = column_sums[CHUNK - 1 :, :]
    later = jnp.exp(total_fading - column_sums)
    since_start = jnp.exp(column_sums)
    between = jnp.exp(jnp.minimum(column_sums - row_sums, 0.0))
    summed = jnp.zeros(out.shape, jnp.float32)
    for group, (queries, keys, switches, state, key_width) in enumerate(
        (
            (queries_a, keys_a, switches_a, state_a, FIRST_KEY_SIZE),
            (queries_b, keys_b, switches_b, state_b, SECOND_KEY_SIZE),
        )
    ):
        width = keys.shape[1]
        sums = channel_sums(switches[...])
        middle = sums[MIDDLE : MIDDLE + 1, :]
        scaled = queries[...].astype(jnp.float32) * (jnp.exp(sums - middle) * key_width**-0.5)
        scaled = scaled.astype(jnp.bfloat16)
        inverse_keys = (keys[...].astype(jnp.float32) * jnp.exp(middle - sums)).astype(jnp.bfloat16)
        before = (state[...] * jnp.exp(middle)).astype(jnp.bfloat16)
        pieces = []
        for h in range(width // key_width):
            here = slice(h * DV, (h + 1) * DV)
            if key_width % 128 == 0:
                mine = slice(h * key_width, (h + 1) * key_width)
                q, k, s = scaled[:, mine], inverse_keys[:, mine], before[:, mine]
            else:
                q = jnp.where(lanes_of(h, width, key_width), scaled, jnp.zeros_like(scaled))
                k, s = inverse_keys, before
            scores = dot(q, k, ((1,), (1,))) * between
            scores = jnp.where(causal, scores, 0.0).astype(jnp.bfloat16)
            head = dot(scores, values[group, :, here], ((1,), (0,)))
            head = head + since_start * dot(q, s, ((1,), (1,)))
            inverse = lax.rsqrt(jnp.mean(head * head, axis=-1, keepdims=True) + EPS)
            gate = gates[group, :, here].astype(jnp.float32)
            silu = gate / (1.0 + jnp.exp(-gate))
            pieces.append((silu * (head * inverse * gains[group : group + 1, here])).astype(jnp.bfloat16))
        gated = pieces[0] if len(pieces) == 1 else jnp.concatenate(pieces, axis=1)
        summed = summed + dot(gated, projection[group], ((1,), (0,)))
        weighted = (values[group].astype(jnp.float32) * later).astype(jnp.bfloat16)
        state[...] = advanced(state[...], inverse_keys, weighted, sums, total_fading, key_width)
    out[...] = summed.astype(out.dtype)


def rows_of(array):
    return pl.BlockSpec((CHUNK, array.shape[1]), lambda i: (i, 0))


def pair_rows_of(array):
    return pl.BlockSpec((2, CHUNK, array.shape[2]), lambda i: (0, i, 0))


def whole(array):
    return pl.BlockSpec(array.shape, lambda i: (0,) * array.ndim)


def attention_terms(qa, ka, qb, kb, sa, sb, fading, values, gates, gains, projection):
    rows = qa.shape[0]
    steps = rows // CHUNK
    width_a, width_b = ka.shape[1], kb.shape[1]
    lines = fading.reshape(steps, 1, CHUNK)
    line_spec = pl.BlockSpec((1, 1, CHUNK), lambda i: (i, 0, 0))
    states = [pltpu.VMEM((DV, width_a), jnp.float32), pltpu.VMEM((DV, width_b), jnp.float32)]
    params = pltpu.CompilerParams(dimension_semantics=("arbitrary",))
    packed = pl.pallas_call(
        state_kernel,
        grid=(steps,),
        in_specs=[rows_of(ka), rows_of(kb), rows_of(sa), rows_of(sb), line_spec, pair_rows_of(values)],
        out_specs=pl.BlockSpec((DV + PAD, width_a + width_b), lambda i: (0, 0)),
        out_shape=jax.ShapeDtypeStruct((DV + PAD, width_a + width_b), jnp.bfloat16),
        scratch_shapes=states + [pltpu.VMEM((8, width_a + width_b), jnp.float32)],
        compiler_params=params,
        cost_estimate=pl.CostEstimate(flops=4_000_000_000, bytes_accessed=8_000_000, transcendentals=0),
        name="states",
    )(ka, kb, sa, sb, lines, values)
    everything = lax.all_gather(packed, "sp")
    place = lax.axis_index("sp").astype(jnp.int32).reshape(1)
    return pl.pallas_call(
        output_kernel,
        grid=(steps,),
        in_specs=[
            pl.BlockSpec(memory_space=pltpu.SMEM),
            whole(everything),
            rows_of(qa),
            rows_of(qb),
            rows_of(ka),
            rows_of(kb),
            rows_of(sa),
            rows_of(sb),
            line_spec,
            pair_rows_of(values),
            pair_rows_of(gates),
            whole(gains),
            whole(projection),
        ],
        out_specs=pl.BlockSpec((CHUNK, projection.shape[2]), lambda i: (i, 0)),
        out_shape=jax.ShapeDtypeStruct((rows, projection.shape[2]), jnp.bfloat16),
        scratch_shapes=states,
        compiler_params=params,
        cost_estimate=pl.CostEstimate(flops=8_000_000_000, bytes_accessed=16_000_000, transcendentals=0),
        name="outputs",
    )(place, everything, qa, qb, ka, kb, sa, sb, lines, values, gates, gains, projection)


def row_norm(source, gain_row):
    widened = source.astype(jnp.float32)
    inverse = lax.rsqrt(jnp.mean(widened * widened, axis=-1, keepdims=True) + EPS)
    return (widened * inverse * gain_row).astype(jnp.bfloat16)


def per_device(
    residual,
    first_group_queries,
    first_group_keys,
    second_group_queries,
    second_group_keys,
    primary_retain_switch_inputs,
    secondary_retain_switch_inputs,
    timestep_fading_exponent,
    values,
    output_gate_logits,
    head_norm_gains,
    output_projection,
    feedforward_norm_gain,
    gate_projection,
    up_projection,
    down_projection,
):
    terms = attention_terms(
        first_group_queries,
        first_group_keys,
        second_group_queries,
        second_group_keys,
        primary_retain_switch_inputs,
        secondary_retain_switch_inputs,
        timestep_fading_exponent,
        values,
        output_gate_logits,
        head_norm_gains,
        output_projection,
    )
    attention = lax.psum_scatter(terms, "tp", scatter_dimension=0, tiled=True).astype(jnp.float32)
    mid_rows = (residual.astype(jnp.float32) + attention).astype(jnp.bfloat16)
    all_rows = lax.all_gather(row_norm(mid_rows, feedforward_norm_gain), "tp", axis=0, tiled=True)
    gate_sum = jnp.dot(
        all_rows,
        lax.all_gather(gate_projection, "sp", axis=0, tiled=True),
        preferred_element_type=jnp.float32,
    )
    up_sum = jnp.dot(
        all_rows,
        lax.all_gather(up_projection, "sp", axis=0, tiled=True),
        preferred_element_type=jnp.float32,
    )
    hidden = (jax.nn.silu(gate_sum) * up_sum).astype(jnp.bfloat16)
    down_terms = jnp.dot(
        hidden,
        lax.all_gather(down_projection, "sp", axis=1, tiled=True),
        preferred_element_type=jnp.float32,
    )
    down_sum = lax.psum_scatter(
        down_terms.astype(jnp.bfloat16), "tp", scatter_dimension=0, tiled=True
    ).astype(jnp.float32)
    return (mid_rows.astype(jnp.float32) + down_sum).astype(jnp.bfloat16)


def solution(mesh):
    return jax.shard_map(
        per_device,
        mesh=mesh,
        in_specs=(
            P(("sp", "tp"), None),
            P("sp", "tp"),
            P("sp", "tp"),
            P("sp", "tp"),
            P("sp", "tp"),
            P("sp", "tp"),
            P("sp", "tp"),
            P("sp"),
            P(None, "sp", "tp"),
            P(None, "sp", "tp"),
            P(None, "tp"),
            P(None, "tp", None),
            P(),
            P("sp", "tp"),
            P("sp", "tp"),
            P("tp", "sp"),
        ),
        out_specs=P(("sp", "tp"), None),
        check_vma=False,
    )
```

```python
import jax
import jax.numpy as jnp
from jax import lax
from jax.experimental import pallas as pl
from jax.experimental.pallas import tpu as pltpu
from jax.sharding import PartitionSpec as P

FIRST_KEY_SIZE = 128
SECOND_KEY_SIZE = 64
DV = 128
CHUNK = 128
MIDDLE = CHUNK // 2 - 1
PAD = 16

EPS = 1e-06
SOFTNESS_SCALE = 16.0
PARTS = 2


def dot(a, b, dims):
    return lax.dot_general(a, b, (dims, ((), ())), preferred_element_type=jnp.float32)


def positions():
    row = lax.broadcasted_iota(jnp.int32, (CHUNK, CHUNK), 0)
    column = lax.broadcasted_iota(jnp.int32, (CHUNK, CHUNK), 1)
    return row, column


def fading_sums(fading_row):
    row, column = positions()
    as_column = jnp.sum(jnp.where(row == column, fading_row, 0.0), axis=1, keepdims=True)
    column_sums = jnp.sum(jnp.where(column <= row, fading_row, 0.0), axis=1, keepdims=True)
    row_sums = jnp.sum(jnp.where(row <= column, as_column, 0.0), axis=0, keepdims=True)
    return column_sums, row_sums


def channel_sums(switches):
    row, column = positions()
    x = switches.astype(jnp.float32)
    logs = (jnp.minimum(x, 0.0) - jnp.log1p(jnp.exp(-jnp.abs(x)))) * (1.0 / SOFTNESS_SCALE)
    lower = (column <= row).astype(jnp.bfloat16)
    high = logs.astype(jnp.bfloat16)
    low = (logs - high.astype(jnp.float32)).astype(jnp.bfloat16)
    return dot(lower, high, ((1,), (0,))) + dot(lower, low, ((1,), (0,)))


def lanes_of(head, width, key_width):
    lane = lax.broadcasted_iota(jnp.int32, (1, width), 1)
    return (lane >= head * key_width) & (lane < (head + 1) * key_width)


def advanced(state, inverse_keys, weighted, sums, total_fading, key_width):
    width = state.shape[1]
    end, middle = sums[CHUNK - 1 :, :], sums[MIDDLE : MIDDLE + 1, :]
    head_count = width // key_width
    if key_width % 128 == 0:
        added = jnp.concatenate(
            [
                dot(
                    weighted[:, h * DV : (h + 1) * DV],
                    inverse_keys[:, h * key_width : (h + 1) * key_width],
                    ((0,), (0,)),
                )
                for h in range(head_count)
            ],
            axis=1,
        )
    else:
        added = jnp.zeros((DV, width), jnp.float32)
        for h in range(head_count):
            product = dot(weighted[:, h * DV : (h + 1) * DV], inverse_keys, ((0,), (0,)))
            added = jnp.where(lanes_of(h, width, key_width), product, added)
    return jnp.exp(end + total_fading) * state + jnp.exp(end - middle) * added


def state_kernel(
    keys_a, keys_b, switches_a, switches_b, fading, values, packed, state_a, state_b, decay
):
    step = pl.program_id(0)
    width_a = keys_a.shape[1]

    @pl.when(step == 0)
    def _():
        state_a[...] = jnp.zeros_like(state_a)
        state_b[...] = jnp.zeros_like(state_b)
        decay[...] = jnp.zeros_like(decay)

    column_sums, _ = fading_sums(fading[0])
    total_fading = column_sums[CHUNK - 1 :, :]
    later = jnp.exp(total_fading - column_sums)
    for group, (keys, switches, state, key_width, start) in enumerate(
        (
            (keys_a, switches_a, state_a, FIRST_KEY_SIZE, 0),
            (keys_b, switches_b, state_b, SECOND_KEY_SIZE, width_a),
        )
    ):
        width = keys.shape[1]
        sums = channel_sums(switches[...])
        middle = sums[MIDDLE : MIDDLE + 1, :]
        inverse_keys = (keys[...].astype(jnp.float32) * jnp.exp(middle - sums)).astype(jnp.bfloat16)
        weighted = (values[group].astype(jnp.float32) * later).astype(jnp.bfloat16)
        state[...] = advanced(state[...], inverse_keys, weighted, sums, total_fading, key_width)
        decay[:, start : start + width] += sums[CHUNK - 1 :, :] + total_fading

    @pl.when(step == pl.num_programs(0) - 1)
    def _():
        packed[:DV, :width_a] = state_a[...].astype(jnp.bfloat16)
        packed[:DV, width_a:] = state_b[...].astype(jnp.bfloat16)
        packed[DV:, :] = jnp.broadcast_to(jnp.exp(decay[:1, :]), (PAD, decay.shape[1])).astype(
            jnp.bfloat16
        )


def output_kernel(
    place,
    everything,
    queries_a,
    queries_b,
    keys_a,
    keys_b,
    switches_a,
    switches_b,
    fading,
    values,
    gates,
    gains,
    projection,
    out,
    state_a,
    state_b,
):
    step = pl.program_id(0)
    width_a = keys_a.shape[1]

    @pl.when(step == 0)
    def _():
        state_a[...] = jnp.zeros_like(state_a)
        state_b[...] = jnp.zeros_like(state_b)

        @pl.loop(0, place[0])
        def _(k):
            part = everything[k].astype(jnp.float32)
            factor = part[DV : DV + 1, :]
            state_a[...] = factor[:, :width_a] * state_a[...] + part[:DV, :width_a]
            state_b[...] = factor[:, width_a:] * state_b[...] + part[:DV, width_a:]

    row, column = positions()
    causal = column <= row
    column_sums, row_sums = fading_sums(fading[0])
    total_fading = column_sums[CHUNK - 1 :, :]
    later = jnp.exp(total_fading - column_sums)
    since_start = jnp.exp(column_sums)
    between = jnp.exp(jnp.minimum(column_sums - row_sums, 0.0))
    summed = jnp.zeros(out.shape, jnp.float32)
    for group, (queries, keys, switches, state, key_width) in enumerate(
        (
            (queries_a, keys_a, switches_a, state_a, FIRST_KEY_SIZE),
            (queries_b, keys_b, switches_b, state_b, SECOND_KEY_SIZE),
        )
    ):
        width = keys.shape[1]
        sums = channel_sums(switches[...])
        middle = sums[MIDDLE : MIDDLE + 1, :]
        scaled = queries[...].astype(jnp.float32) * (jnp.exp(sums - middle) * key_width**-0.5)
        scaled = scaled.astype(jnp.bfloat16)
        inverse_keys = (keys[...].astype(jnp.float32) * jnp.exp(middle - sums)).astype(jnp.bfloat16)
        before = (state[...] * jnp.exp(middle)).astype(jnp.bfloat16)
        pieces = []
        for h in range(width // key_width):
            here = slice(h * DV, (h + 1) * DV)
            if key_width % 128 == 0:
                mine = slice(h * key_width, (h + 1) * key_width)
                q, k, s = scaled[:, mine], inverse_keys[:, mine], before[:, mine]
            else:
                q = jnp.where(lanes_of(h, width, key_width), scaled, jnp.zeros_like(scaled))
                k, s = inverse_keys, before
            scores = dot(q, k, ((1,), (1,))) * between
            scores = jnp.where(causal, scores, 0.0).astype(jnp.bfloat16)
            head = dot(scores, values[group, :, here], ((1,), (0,)))
            head = head + since_start * dot(q, s, ((1,), (1,)))
            inverse = lax.rsqrt(jnp.mean(head * head, axis=-1, keepdims=True) + EPS)
            gate = gates[group, :, here].astype(jnp.float32)
            silu = gate / (1.0 + jnp.exp(-gate))
            pieces.append((silu * (head * inverse * gains[group : group + 1, here])).astype(jnp.bfloat16))
        gated = pieces[0] if len(pieces) == 1 else jnp.concatenate(pieces, axis=1)
        summed = summed + dot(gated, projection[group], ((1,), (0,)))
        weighted = (values[group].astype(jnp.float32) * later).astype(jnp.bfloat16)
        state[...] = advanced(state[...], inverse_keys, weighted, sums, total_fading, key_width)
    out[...] = summed.astype(out.dtype)


def rows_of(array):
    return pl.BlockSpec((CHUNK, array.shape[1]), lambda i: (i, 0))


def pair_rows_of(array):
    return pl.BlockSpec((2, CHUNK, array.shape[2]), lambda i: (0, i, 0))


def whole(array):
    return pl.BlockSpec(array.shape, lambda i: (0,) * array.ndim)


def attention_terms(qa, ka, qb, kb, sa, sb, fading, values, gates, gains, projection):
    rows = qa.shape[0]
    steps = rows // CHUNK
    width_a, width_b = ka.shape[1], kb.shape[1]
    lines = fading.reshape(steps, 1, CHUNK)
    line_spec = pl.BlockSpec((1, 1, CHUNK), lambda i: (i, 0, 0))
    states = [pltpu.VMEM((DV, width_a), jnp.float32), pltpu.VMEM((DV, width_b), jnp.float32)]
    params = pltpu.CompilerParams(dimension_semantics=("arbitrary",))
    packed = pl.pallas_call(
        state_kernel,
        grid=(steps,),
        in_specs=[rows_of(ka), rows_of(kb), rows_of(sa), rows_of(sb), line_spec, pair_rows_of(values)],
        out_specs=pl.BlockSpec((DV + PAD, width_a + width_b), lambda i: (0, 0)),
        out_shape=jax.ShapeDtypeStruct((DV + PAD, width_a + width_b), jnp.bfloat16),
        scratch_shapes=states + [pltpu.VMEM((8, width_a + width_b), jnp.float32)],
        compiler_params=params,
        cost_estimate=pl.CostEstimate(flops=4_000_000_000, bytes_accessed=8_000_000, transcendentals=0),
        name="states",
    )(ka, kb, sa, sb, lines, values)
    everything = lax.all_gather(packed, "sp")
    place = lax.axis_index("sp").astype(jnp.int32).reshape(1)
    return pl.pallas_call(
        output_kernel,
        grid=(steps,),
        in_specs=[
            pl.BlockSpec(memory_space=pltpu.SMEM),
            whole(everything),
            rows_of(qa),
            rows_of(qb),
            rows_of(ka),
            rows_of(kb),
            rows_of(sa),
            rows_of(sb),
            line_spec,
            pair_rows_of(values),
            pair_rows_of(gates),
            whole(gains),
            whole(projection),
        ],
        out_specs=pl.BlockSpec((CHUNK, projection.shape[2]), lambda i: (i, 0)),
        out_shape=jax.ShapeDtypeStruct((rows, projection.shape[2]), jnp.bfloat16),
        scratch_shapes=states,
        compiler_params=params,
        cost_estimate=pl.CostEstimate(flops=8_000_000_000, bytes_accessed=16_000_000, transcendentals=0),
        name="outputs",
    )(place, everything, qa, qb, ka, kb, sa, sb, lines, values, gates, gains, projection)


def scatter_sum(terms, axis):
    peers, place = lax.axis_size(axis), lax.axis_index(axis)
    rows = terms.shape[0] // peers

    def block(k):
        return lax.dynamic_slice_in_dim(terms, lax.rem(place + k, peers) * rows, rows, 0)

    total = block(0).astype(jnp.float32)
    for k in range(1, peers):
        moves = [(i, (i + k) % peers) for i in range(peers)]
        total = total + lax.ppermute(block(k), axis, moves).astype(jnp.float32)
    return total


def gather_rows(own, axis):
    peers, place = lax.axis_size(axis), lax.axis_index(axis)
    rows = own.shape[0]
    full = jnp.zeros((rows * peers, own.shape[1]), own.dtype)
    full = lax.dynamic_update_slice_in_dim(full, own, place * rows, 0)
    for k in range(1, peers):
        moves = [(i, (i + k) % peers) for i in range(peers)]
        arrived = lax.ppermute(own, axis, moves)
        at = lax.rem(place - k + peers, peers) * rows
        full = lax.dynamic_update_slice_in_dim(full, arrived, at, 0)
    return full


def ring_places(peers):
    order = list(range(0, peers, 2)) + list(range(1, peers, 2))[::-1]
    at = [0] * peers
    for position, index in enumerate(order):
        at[index] = position
    return order, at


def ring_gather(own, axis):
    peers = lax.axis_size(axis)
    order, _ = ring_places(peers)
    forward = [(order[i], order[(i + 1) % peers]) for i in range(peers)]
    backward = [(order[i], order[i - 1]) for i in range(peers)]
    held = [own] * peers
    ahead, behind = peers // 2, peers - 1 - peers // 2
    for k in range(1, ahead + 1):
        held[k] = lax.ppermute(held[k - 1], axis, forward)
        if k <= behind:
            held[peers - k] = lax.ppermute(held[(peers - k + 1) % peers], axis, backward)
    return held


def in_order(blocks, axis):
    peers = lax.axis_size(axis)
    _, at = ring_places(peers)
    mine = jnp.asarray(at, jnp.int32)[lax.axis_index(axis)]
    stacked = jnp.stack(blocks)
    return jnp.concatenate(
        [
            lax.dynamic_index_in_dim(stacked, lax.rem(mine - at[s] + peers, peers), 0, keepdims=False)
            for s in range(peers)
        ],
        axis=1,
    )


def row_norm(source, gain_row):
    widened = source.astype(jnp.float32)
    inverse = lax.rsqrt(jnp.mean(widened * widened, axis=-1, keepdims=True) + EPS)
    return (widened * inverse * gain_row).astype(jnp.bfloat16)


def per_device(
    residual,
    first_group_queries,
    first_group_keys,
    second_group_queries,
    second_group_keys,
    primary_retain_switch_inputs,
    secondary_retain_switch_inputs,
    timestep_fading_exponent,
    values,
    output_gate_logits,
    head_norm_gains,
    output_projection,
    feedforward_norm_gain,
    gate_projection,
    up_projection,
    down_projection,
):
    terms = attention_terms(
        first_group_queries,
        first_group_keys,
        second_group_queries,
        second_group_keys,
        primary_retain_switch_inputs,
        secondary_retain_switch_inputs,
        timestep_fading_exponent,
        values,
        output_gate_logits,
        head_norm_gains,
        output_projection,
    )
    down_blocks = ring_gather(down_projection, "sp")
    gate_matrix = lax.all_gather(gate_projection, "sp", axis=0, tiled=True)
    up_matrix = lax.all_gather(up_projection, "sp", axis=0, tiled=True)
    mid_rows = (residual.astype(jnp.float32) + scatter_sum(terms, "tp")).astype(jnp.bfloat16)
    all_rows = gather_rows(row_norm(mid_rows, feedforward_norm_gain), "tp")
    gate_sum = jnp.dot(all_rows, gate_matrix, preferred_element_type=jnp.float32)
    up_sum = jnp.dot(all_rows, up_matrix, preferred_element_type=jnp.float32)
    hidden = (jax.nn.silu(gate_sum) * up_sum).astype(jnp.bfloat16)
    peers, columns = lax.axis_size("sp"), down_projection.shape[1]
    count = peers // PARTS if peers % PARTS == 0 else peers
    blocks = []
    for first in range(0, peers, count):
        down_matrix = jnp.concatenate(down_blocks[first : first + count], axis=1)
        down_terms = jnp.dot(hidden, down_matrix, preferred_element_type=jnp.float32)
        down_sum = scatter_sum(down_terms.astype(jnp.bfloat16), "tp")
        blocks += [down_sum[:, k * columns : (k + 1) * columns] for k in range(count)]
    down_sum = in_order(blocks, "sp")
    return (mid_rows.astype(jnp.float32) + down_sum).astype(jnp.bfloat16)


def solution(mesh):
    return jax.shard_map(
        per_device,
        mesh=mesh,
        in_specs=(
            P(("sp", "tp"), None),
            P("sp", "tp"),
            P("sp", "tp"),
            P("sp", "tp"),
            P("sp", "tp"),
            P("sp", "tp"),
            P("sp", "tp"),
            P("sp"),
            P(None, "sp", "tp"),
            P(None, "sp", "tp"),
            P(None, "tp"),
            P(None, "tp", None),
            P(),
            P("sp", "tp"),
            P("sp", "tp"),
            P("tp", "sp"),
        ),
        out_specs=P(("sp", "tp"), None),
        check_vma=False,
    )
```
